32 devices in a mesh: rep: 2 (over y), fs: 4 (over z), tp: 4 (over x, core).
Axes of the slice: x: 2, y: 2, z: 4, core: 2. Of those that a mesh axis runs over, the one named last changes fastest.
Arguments:
- tokens: bfloat16 [4096, 2048], P(('rep', 'fs', 'tp')), may hold values from -6 to 6
- norm_gain: float32 [2048], replicated, may hold values from 0.1 to 1.9
- w_gate: bfloat16 [2048, 3072], P('fs', 'tp'), may hold values from -0.125 to 0.125
- w_up: bfloat16 [2048, 3072], P('fs', 'tp'), may hold values from -0.125 to 0.125
- w_down: bfloat16 [3072, 2048], P('tp', 'fs'), may hold values from -0.109375 to 0.109375
- post_gain: float32 [2048], replicated, may hold values from 0.1 to 1.9
Outputs:
- result: bfloat16 [4096, 2048], P(('rep', 'fs', 'tp'))
The draws below stay inside these ranges and needn't reach their ends.
All inputs are finite; a program needn't handle non-finite values.
Results may differ from the reference program's by a relative error of at most 0.014.
Values may be sent and summed in bfloat16 or wider, within the bound.
A program may use at most 64 MiB of HBM per device.

```python
import jax
import jax.numpy as jnp
from jax import lax

D = 2048
FF = 3072
TOKENS = 4096
N_TP = 4


def block_scale(own_key, dims, split, smallest, top_value):
    level, own = 1.0, jax.random.fold_in(own_key, 6)
    for axis_at, blocks in split:
        heights = jnp.exp(jax.random.uniform(jax.random.fold_in(own, axis_at), (blocks,), jnp.float32, smallest / len(split), top_value / len(split)))
        level = level * jnp.repeat(heights, dims[axis_at] // blocks).reshape([-1 if axis == axis_at else 1 for axis in range(len(dims))])
    return level


def bell_draw(rng, dims, width, limit, split=(), held_as=jnp.bfloat16):
    values = width * jax.random.normal(rng, dims, jnp.float32)
    if split:
        values = values * block_scale(rng, dims, split, -0.22, 0.18)
    return jnp.clip(values, -limit, limit).astype(held_as)


def setup_inputs(seed: int = 0) -> dict:
    streams_of = jax.random.split(jax.random.key(seed), 7)
    return {
        "tokens": bell_draw(streams_of[0], (TOKENS, D), 1.0, 6.0, ((0, 32),)),
        "norm_gain": jnp.clip(1.0 + 0.18 * jax.random.normal(streams_of[1], (D,), jnp.float32), 0.1, 1.9),
        "w_gate": bell_draw(streams_of[2], (D, FF), D ** -0.5, 0.125, ((0, 4), (1, 4))),
        "w_up": bell_draw(streams_of[3], (D, FF), D ** -0.5, 0.125, ((0, 4), (1, 4))),
        "w_down": bell_draw(streams_of[4], (FF, D), FF ** -0.5, 0.109375, ((0, 4), (1, 4))),
        "post_gain": jnp.clip(1.0 + 0.18 * jax.random.normal(streams_of[5], (D,), jnp.float32), 0.1, 1.9),
    }


EPS = 1e-06

def rms_scale(values, gain):
    return values * lax.rsqrt(lax.optimization_barrier(jnp.mean(values * values, axis=-1, keepdims=True)) + EPS) * gain

def reference(tokens, norm_gain, w_gate, w_up, w_down, post_gain):
    normed = rms_scale(tokens.astype(jnp.float32), norm_gain).astype(jnp.bfloat16)
    gate = jnp.dot(normed, w_gate, preferred_element_type=jnp.float32)
    up = jnp.dot(normed, w_up, preferred_element_type=jnp.float32)
    hidden = (jax.nn.silu(gate) * up).astype(jnp.bfloat16)
    block = FF // N_TP
    summed = jnp.zeros((tokens.shape[0], D), jnp.float32)
    for index in range(N_TP):
        partial_block = jnp.dot(hidden[:, index * block:(index + 1) * block], w_down[index * block:(index + 1) * block], preferred_element_type=jnp.float32).astype(jnp.bfloat16)
        partial_block = lax.optimization_barrier(partial_block)
        summed = summed + partial_block.astype(jnp.float32)
    return rms_scale(summed, post_gain).astype(jnp.bfloat16)
```

```python
import functools

import jax
import jax.numpy as jnp
from jax import lax
from jax.experimental import pallas as pl
from jax.experimental.pallas import tpu as pltpu
from jax.sharding import PartitionSpec as P

EPS = 1e-06
MESH = pl.DeviceIdType.MESH


def rms_scale(values, gain):
    return values * lax.rsqrt(jnp.mean(values * values, axis=-1, keepdims=True) + EPS) * gain


def plain_body(tokens, norm_gain, w_gate, w_up, w_down, post_gain):
    own_normed = rms_scale(tokens.astype(jnp.float32), norm_gain).astype(jnp.bfloat16)
    normed = lax.all_gather(own_normed, "tp", axis=0, tiled=True)
    gate = jnp.dot(
        normed, lax.all_gather(w_gate, "fs", axis=0, tiled=True), preferred_element_type=jnp.float32
    )
    up = jnp.dot(
        normed, lax.all_gather(w_up, "fs", axis=0, tiled=True), preferred_element_type=jnp.float32
    )
    hidden = (jax.nn.silu(gate) * up).astype(jnp.bfloat16)
    terms = jnp.dot(
        hidden, lax.all_gather(w_down, "fs", axis=1, tiled=True), preferred_element_type=jnp.float32
    )
    summed = lax.psum_scatter(
        terms.astype(jnp.bfloat16), "tp", scatter_dimension=0, tiled=True
    ).astype(jnp.float32)
    return rms_scale(summed, post_gain).astype(jnp.bfloat16)


def kernel(
    n, rows, depth, part, width,
    tok_ref, gain_ref, wg_ref, wu_ref, wd_ref, post_ref, out_ref,
    raw, normed, gu, dn, hidden, kept, pair_out, pair_in, cross_out, cross_in, fin,
    loc_sem, tok_s, tok_r, w_s, w_r, pair_s, pair_r, cross_s, cross_r,
):
    r, k, t = lax.axis_index("rep"), lax.axis_index("fs"), lax.axis_index("tp")
    x, c = t // 2, t % 2
    t_pair, t_x, r_y = x * 2 + (1 - c), (1 - x) * 2 + c, 1 - r
    partner, along_x, along_y, diag = {"tp": t_pair}, {"tp": t_x}, {"rep": r_y}, {"rep": r_y, "tp": t_x}
    has_left, has_right = k > 0, k < n - 1

    def weight(s, q):
        if q < 2:
            return gu.at[pl.ds(s * depth, depth), pl.ds(q * part, part)]
        return dn.at[s]

    half = pl.multiple_of(r * part, part)
    loads = [
        pltpu.make_async_copy(wg_ref.at[:, pl.ds(half, part)], weight(k, 0), loc_sem.at[0]),
        pltpu.make_async_copy(wu_ref.at[:, pl.ds(half, part)], weight(k, 1), loc_sem.at[1]),
        pltpu.make_async_copy(wd_ref.at[pl.ds(half, part), :], weight(k, 2), loc_sem.at[2]),
        pltpu.make_async_copy(tok_ref, raw.at[pl.ds((r * 4 + t) * rows, rows)], loc_sem.at[3]),
    ]
    for load in loads:
        load.start()

    barrier = pltpu.get_barrier_semaphore()
    for where in (partner, along_x, along_y, diag):
        pl.semaphore_signal(barrier, inc=1, device_id=where, device_id_type=MESH)

    @pl.when(has_left)
    def _():
        pl.semaphore_signal(barrier, inc=1, device_id={"fs": k - 1}, device_id_type=MESH)

    @pl.when(has_right)
    def _():
        pl.semaphore_signal(barrier, inc=1, device_id={"fs": k + 1}, device_id_type=MESH)

    pl.semaphore_wait(barrier, 4 + jnp.where(has_left, 1, 0) + jnp.where(has_right, 1, 0))

    def remote(ref, send, recv, where):
        return pltpu.make_async_remote_copy(ref, ref, send, recv, device_id=where, device_id_type=MESH)

    def hop(way, s, q):
        return remote(weight(s, q), w_s.at[way, s, q], w_r.at[s, q], {"fs": k + 1 - 2 * way})

    def pass_on(way, s, q):
        @pl.when(has_left if way else has_right)
        def _():
            hop(way, s, q).start()

    def rows_of(r_at, t_at, first=0, count=rows):
        return raw.at[pl.ds((r_at * 4 + t_at) * rows + first, count)]

    upper = rows // 2
    token_sends = [
        (rows_of(r, t), partner),
        (rows_of(r, t), along_x),
        (rows_of(r, t), along_y),
        (rows_of(r, t_x, 0, upper), along_y),
        (rows_of(r_y, t, upper, upper), along_x),
        (rows_of(r, t_x), partner),
        (rows_of(r_y, t), partner),
        (rows_of(r_y, t_x), partner),
    ]
    t_px = (1 - x) * 2 + (1 - c)
    token_lands = [
        rows_of(r, t_pair),
        rows_of(r, t_x),
        rows_of(r_y, t),
        rows_of(r_y, t_x, 0, upper),
        rows_of(r_y, t_x, upper, upper),
        rows_of(r, t_px),
        rows_of(r_y, t_pair),
        rows_of(r_y, t_px),
    ]

    def token_send(i):
        ref, where = token_sends[i]
        return remote(ref, tok_s.at[i], tok_r.at[i], where)

    def token_wait(i):
        remote(token_lands[i], tok_s.at[i], tok_r.at[i], partner).wait_recv()

    loads[3].wait()
    for i in (1, 2, 0):
        token_send(i).start()
    for q in (0, 1):
        loads[q].wait()
        pass_on(0, k, q)
        pass_on(1, k, q)

    def arrive(step, q):
        for way, s in ((0, k - step), (1, k + step)):
            @pl.when((s >= 0) if way == 0 else (s < n))
            def _():
                hop(way, s, q).wait_recv()
                pass_on(way, s, q)

    def forward_tokens():
        token_wait(1)
        token_send(3).start()
        token_send(5).start()
        token_wait(2)
        token_send(4).start()
        token_send(6).start()

    def finish_tokens():
        token_wait(3)
        token_wait(4)
        token_send(7).start()
        for i in (0, 5, 6, 7):
            token_wait(i)

        tile = 32

        @pl.loop(0, 8 * rows // tile)
        def _(i):
            at = pl.ds(pl.multiple_of(i * tile, tile), tile)
            normed[at, :] = rms_scale(raw[at, :].astype(jnp.float32), gain_ref[...]).astype(jnp.bfloat16)

    for step in range(1, n):
        arrive(step, 0)
        if step == 1:
            forward_tokens()
        arrive(step, 1)
        if step == 1:
            finish_tokens()

    loads[2].wait()
    pass_on(0, k, 2)
    pass_on(1, k, 2)

    tile = 2 * rows

    @pl.loop(0, 4)
    def _(i):
        at = pl.ds(pl.multiple_of(i * tile, tile), tile)
        both = jnp.dot(normed[at, :], gu[...], preferred_element_type=jnp.float32)
        gate, up = both[:, :part], both[:, part:]
        hidden[at, :] = (gate / (1.0 + jnp.exp(-gate)) * up).astype(jnp.bfloat16)

    mine = r * 2 + x
    others = ((r * 2 + (1 - x), along_x), (r_y * 2 + x, along_y), (r_y * 2 + (1 - x), diag))

    def pair_copy(s):
        return pltpu.make_async_remote_copy(
            pair_out.at[s], pair_in.at[s], pair_s.at[s], pair_r.at[s], device_id=partner, device_id_type=MESH
        )

    def cross_copy(s, to, where):
        return pltpu.make_async_remote_copy(
            cross_out.at[s, to], cross_in.at[s, mine], cross_s.at[s, to], cross_r.at[s, mine],
            device_id=where, device_id_type=MESH,
        )

    def reduce_block(s):
        @pl.loop(0, 4)
        def _(m):
            at = pl.ds(pl.multiple_of((m * 2 + (1 - c)) * rows, rows), rows)
            pair_out[s, m] = jnp.dot(
                hidden[at, :], dn[s], preferred_element_type=jnp.float32
            ).astype(jnp.bfloat16)

        pair_copy(s).start()

        @pl.loop(0, 4)
        def _(m):
            at = pl.ds(pl.multiple_of((m * 2 + c) * rows, rows), rows)
            kept[m] = jnp.dot(hidden[at, :], dn[s], preferred_element_type=jnp.float32)

        pair_copy(s).wait_recv()
        for to, where in others:
            cross_out[s, to] = (kept[to] + pair_in[s, to].astype(jnp.float32)).astype(jnp.bfloat16)
        for to, where in (others[2], others[0], others[1]):
            cross_copy(s, to, where).start()
        fin[s] = kept[mine] + pair_in[s, mine].astype(jnp.float32)

    reduce_block(k)
    for step in range(1, n):
        arrive(step, 2)
        for s in (k - step, k + step):
            @pl.when((s >= 0) & (s < n))
            def _():
                reduce_block(s)

    def take(i):
        for s_at in range(n):
            for other, _ in others:
                pltpu.make_async_remote_copy(
                    cross_out.at[s_at, 0], cross_in.at[s_at, other], cross_s.at[s_at, 0],
                    cross_r.at[s_at, other], device_id=along_x, device_id_type=MESH,
                ).wait_recv()

    take(0)
    piece = 32

    @pl.loop(0, rows // piece)
    def _(i):
        at = pl.ds(pl.multiple_of(i * piece, piece), piece)
        blocks = []
        for s in range(n):
            total = fin[s, at, :]
            for other, _ in others:
                total = total + cross_in[s, other, at, :].astype(jnp.float32)
            blocks.append(total)
        square = sum(jnp.sum(b * b, axis=-1, keepdims=True) for b in blocks)
        scale = lax.rsqrt(square / (n * width) + EPS)
        for s in range(n):
            cols = pl.ds(s * width, width)
            out_ref[at, cols] = (blocks[s] * scale * post_ref[:, cols]).astype(out_ref.dtype)

    for i in range(8):
        token_send(i).wait_send()
    for s in range(n):
        for q in range(3):
            @pl.when(has_right & (s <= k))
            def _():
                hop(0, s, q).wait_send()

            @pl.when(has_left & (s >= k))
            def _():
                hop(1, s, q).wait_send()
        pair_copy(s).wait_send()
        for to, where in others:
            cross_copy(s, to, where).wait_send()


def chain_body(n, tokens, norm_gain, w_gate, w_up, w_down, post_gain):
    rows, model = tokens.shape
    depth, block = w_gate.shape
    width = w_down.shape[1]
    part = block // 2
    vmem, dma = pltpu.VMEM, pltpu.SemaphoreType.DMA
    low, full = jnp.bfloat16, jnp.float32
    anywhere = pl.BlockSpec(memory_space=pl.ANY)
    inside = pl.BlockSpec(memory_space=vmem)
    return pl.pallas_call(
        functools.partial(kernel, n, rows, depth, part, width),
        out_shape=jax.ShapeDtypeStruct((rows, model), low),
        in_specs=[anywhere, inside, anywhere, anywhere, anywhere, inside],
        out_specs=inside,
        scratch_shapes=[
            vmem((8 * rows, model), low),
            vmem((8 * rows, model), low),
            vmem((n * depth, 2 * part), low),
            vmem((n, part, width), low),
            vmem((8 * rows, part), low),
            vmem((4, rows, width), full),
            vmem((n, 4, rows, width), low),
            vmem((n, 4, rows, width), low),
            vmem((n, 4, rows, width), low),
            vmem((n, 4, rows, width), low),
            vmem((n, rows, width), full),
            dma((4,)),
            dma((8,)),
            dma((8,)),
            dma((2, n, 3)),
            dma((n, 3)),
            dma((n,)),
            dma((n,)),
            dma((n, 4)),
            dma((n, 4)),
        ],
        compiler_params=pltpu.CompilerParams(
            collective_id=0, has_side_effects=True, vmem_limit_bytes=56 * 2**20
        ),
    )(tokens, norm_gain.reshape(1, -1), w_gate, w_up, w_down, post_gain.reshape(1, -1))


def solution(mesh):
    n = mesh.shape["fs"]

    def body(tokens, norm_gain, w_gate, w_up, w_down, post_gain):
        args = (tokens, norm_gain, w_gate, w_up, w_down, post_gain)
        rows = tokens.shape[0]
        fits = (
            mesh.shape["rep"] == 2 and mesh.shape["tp"] == 4 and 2 <= n <= 4 and rows <= 128
            and rows % 64 == 0 and w_gate.shape[1] % 256 == 0 and w_down.shape[1] % 128 == 0
        )
        return chain_body(n, *args) if fits else plain_body(*args)

    return jax.shard_map(
        body,
        mesh=mesh,
        in_specs=(
            P(("rep", "fs", "tp"), None),
            P(),
            P("fs", "tp"),
            P("fs", "tp"),
            P("tp", "fs"),
            P(),
        ),
        out_specs=P(("rep", "fs", "tp"), None),
        check_vma=False,
    )
```

```python
import functools

import jax
import jax.numpy as jnp
from jax import lax
from jax.experimental import pallas as pl
from jax.experimental.pallas import tpu as pltpu
from jax.sharding import PartitionSpec as P

EPS = 1e-06
MESH = pl.DeviceIdType.MESH
PIECE = 256


def rms_scale(values, gain):
    return values * lax.rsqrt(jnp.mean(values * values, axis=-1, keepdims=True) + EPS) * gain


def plain_body(tokens, norm_gain, w_gate, w_up, w_down, post_gain):
    own_normed = rms_scale(tokens.astype(jnp.float32), norm_gain).astype(jnp.bfloat16)
    normed = lax.all_gather(own_normed, "tp", axis=0, tiled=True)
    gate = jnp.dot(
        normed, lax.all_gather(w_gate, "fs", axis=0, tiled=True), preferred_element_type=jnp.float32
    )
    up = jnp.dot(
        normed, lax.all_gather(w_up, "fs", axis=0, tiled=True), preferred_element_type=jnp.float32
    )
    hidden = (jax.nn.silu(gate) * up).astype(jnp.bfloat16)
    terms = jnp.dot(
        hidden, lax.all_gather(w_down, "fs", axis=1, tiled=True), preferred_element_type=jnp.float32
    )
    summed = lax.psum_scatter(
        terms.astype(jnp.bfloat16), "tp", scatter_dimension=0, tiled=True
    ).astype(jnp.float32)
    return rms_scale(summed, post_gain).astype(jnp.bfloat16)


def kernel(
    n, rows, depth, part, width, cuts,
    tok_ref, gain_ref, wg_ref, wu_ref, wd_ref, post_ref, out_ref,
    raw, normed, acc, gu, dn, hidden, kept, pair_out, pair_in, cross_out, cross_in, fin,
    loc_sem, tok_s, tok_r, w_s, w_r, pair_s, pair_r, cross_s, cross_r,
):
    r, k, t = lax.axis_index("rep"), lax.axis_index("fs"), lax.axis_index("tp")
    x, c = t // 2, t % 2
    t_pair, t_x, r_y = x * 2 + (1 - c), (1 - x) * 2 + c, 1 - r
    partner, along_x, along_y, diag = {"tp": t_pair}, {"tp": t_x}, {"rep": r_y}, {"rep": r_y, "tp": t_x}
    has_left, has_right = k > 0, k < n - 1

    def weight(s, q):
        if isinstance(q, int) and q < 2:
            return gu.at[s, :, pl.ds(q * part, part)]
        return dn.at[s, q - 2]

    sub = width // cuts
    half = pl.multiple_of(r * part, part)
    loads = [
        pltpu.make_async_copy(wg_ref.at[:, pl.ds(half, part)], weight(k, 0), loc_sem.at[0]),
        pltpu.make_async_copy(wu_ref.at[:, pl.ds(half, part)], weight(k, 1), loc_sem.at[1]),
        pltpu.make_async_copy(tok_ref, raw.at[pl.ds((r * 4 + t) * rows, rows)], loc_sem.at[2]),
    ] + [
        pltpu.make_async_copy(
            wd_ref.at[pl.ds(half, part), pl.ds(j * sub, sub)], dn.at[k, j], loc_sem.at[3 + j]
        )
        for j in range(cuts)
    ]
    for load in loads:
        load.start()

    barrier = pltpu.get_barrier_semaphore()
    for where in (partner, along_x, along_y, diag):
        pl.semaphore_signal(barrier, inc=1, device_id=where, device_id_type=MESH)

    @pl.when(has_left)
    def _():
        pl.semaphore_signal(barrier, inc=1, device_id={"fs": k - 1}, device_id_type=MESH)

    @pl.when(has_right)
    def _():
        pl.semaphore_signal(barrier, inc=1, device_id={"fs": k + 1}, device_id_type=MESH)

    pl.semaphore_wait(barrier, 4 + jnp.where(has_left, 1, 0) + jnp.where(has_right, 1, 0))

    def remote(ref, send, recv, where):
        return pltpu.make_async_remote_copy(ref, ref, send, recv, device_id=where, device_id_type=MESH)

    def hop(way, s, q):
        return remote(weight(s, q), w_s.at[way, s, q], w_r.at[s, q], {"fs": k + 1 - 2 * way})

    def pass_on(way, s, q):
        @pl.when(has_left if way else has_right)
        def _():
            hop(way, s, q).start()

    def rows_of(r_at, t_at, first=0, count=rows):
        return raw.at[pl.ds((r_at * 4 + t_at) * rows + first, count)]

    upper = rows // 2
    token_sends = [
        (rows_of(r, t), partner),
        (rows_of(r, t), along_x),
        (rows_of(r, t), along_y),
        (rows_of(r, t_x, 0, upper), along_y),
        (rows_of(r_y, t, upper, upper), along_x),
        (rows_of(r, t_x), partner),
        (rows_of(r_y, t), partner),
        (rows_of(r_y, t_x), partner),
    ]
    t_px = (1 - x) * 2 + (1 - c)
    token_lands = [
        rows_of(r, t_pair),
        rows_of(r, t_x),
        rows_of(r_y, t),
        rows_of(r_y, t_x, 0, upper),
        rows_of(r_y, t_x, upper, upper),
        rows_of(r, t_px),
        rows_of(r_y, t_pair),
        rows_of(r_y, t_px),
    ]

    def token_send(i):
        ref, where = token_sends[i]
        return remote(ref, tok_s.at[i], tok_r.at[i], where)

    def token_wait(i):
        remote(token_lands[i], tok_s.at[i], tok_r.at[i], partner).wait_recv()

    loads[2].wait()
    for i in (1, 2, 0):
        token_send(i).start()
    for q in (0, 1):
        loads[q].wait()
        pass_on(0, k, q)
        pass_on(1, k, q)
    for load in loads[3:]:
        load.wait()

    def start_down(step):
        for way, distance in ((0, k), (1, n - 1 - k)):
            @pl.when(distance == step)
            def _():
                for j in range(cuts):
                    pass_on(way, k, 2 + j)

    start_down(0)

    def arrive(step, q):
        for way, s in ((0, k - step), (1, k + step)):
            @pl.when((s >= 0) if way == 0 else (s < n))
            def _():
                hop(way, s, q).wait_recv()
                pass_on(way, s, q)

    def forward_tokens():
        token_wait(1)
        token_send(3).start()
        token_send(5).start()
        token_wait(2)
        token_send(4).start()
        token_send(6).start()

    def finish_tokens():
        token_wait(3)
        token_wait(4)
        token_send(7).start()
        for i in (0, 5, 6, 7):
            token_wait(i)

        tile = 32

        @pl.loop(0, 8 * rows // tile)
        def _(i):
            at = pl.ds(pl.multiple_of(i * tile, tile), tile)
            normed[at, :] = rms_scale(raw[at, :].astype(jnp.float32), gain_ref[...]).astype(jnp.bfloat16)

    tile = 2 * rows

    def add_block(s, first):
        cols = pl.ds(pl.multiple_of(s * depth, depth), depth)

        @pl.loop(0, 4)
        def _(i):
            at = pl.ds(pl.multiple_of(i * tile, tile), tile)
            term = jnp.dot(normed[at, cols], gu[s], preferred_element_type=jnp.float32)
            acc[at, :] = term if first else acc[at, :] + term

    for step in range(1, n):
        arrive(step, 0)
        if step == 1:
            forward_tokens()
        arrive(step, 1)
        start_down(step)
        if step == 1:
            finish_tokens()
            add_block(k, True)
        for s in (k - step, k + step):
            @pl.when((s >= 0) & (s < n))
            def _():
                add_block(s, False)

    @pl.loop(0, 16)
    def _(i):
        at = pl.ds(pl.multiple_of(i * (rows // 2), rows // 2), rows // 2)
        gate, up = acc[at, :part], acc[at, part:]
        hidden[at, :] = (gate / (1.0 + jnp.exp(-gate)) * up).astype(jnp.bfloat16)

    mine = r * 2 + x
    others = ((r * 2 + (1 - x), along_x), (r_y * 2 + x, along_y), (r_y * 2 + (1 - x), diag))

    def pair_copy(p):
        return pltpu.make_async_remote_copy(
            pair_out.at[p], pair_in.at[p], pair_s.at[p], pair_r.at[p], device_id=partner, device_id_type=MESH
        )

    def cross_copy(p, to, where):
        return pltpu.make_async_remote_copy(
            cross_out.at[p, to], cross_in.at[p, mine], cross_s.at[p, to], cross_r.at[p, mine],
            device_id=where, device_id_type=MESH,
        )

    both_ways = jnp.minimum(k, n - 1 - k)
    far = jnp.where(k < n - 1 - k, 1, -1)

    def source(i):
        near = jnp.where(i % 2 == 1, k - (i + 1) // 2, k + i // 2)
        return jnp.where(i <= 2 * both_ways, near, k + far * (i - both_ways))

    def product(m, core, s, j):
        at = pl.ds(pl.multiple_of((m * 2 + core) * rows, rows), rows)
        return jnp.dot(hidden[at, :], dn[s, j], preferred_element_type=jnp.float32)

    def finish(i, j, slot):
        p = source(i) * cuts + j
        pair_copy(p).wait_recv()
        for to, where in (others[2], others[0], others[1]):
            cross_out[p, to] = (kept[slot, to] + pair_in[p, to].astype(jnp.float32)).astype(jnp.bfloat16)
        for to, where in (others[2], others[0], others[1]):
            cross_copy(p, to, where).start()
        fin[p] = kept[slot, mine] + pair_in[p, mine].astype(jnp.float32)

    @pl.loop(0, n * cuts)
    def _(at):
        i, j, slot = at // cuts, at % cuts, at % 2
        s = source(i)
        p = s * cuts + j

        @pl.when(i > 0)
        def _():
            remote(dn.at[s, j], w_s.at[0, s, 2 + j], w_r.at[s, 2 + j], partner).wait_recv()

        @pl.when((i > 0) & (s < k))
        def _():
            pass_on(0, s, 2 + j)

        @pl.when((i > 0) & (s > k))
        def _():
            pass_on(1, s, 2 + j)

        @pl.loop(0, 4)
        def _(m):
            pair_out[p, m] = product(m, 1 - c, s, j).astype(jnp.bfloat16)

        pair_copy(p).start()

        @pl.loop(0, 4)
        def _(m):
            kept[slot, m] = product(m, c, s, j)

        @pl.when(at > 0)
        def _():
            finish((at - 1) // cuts, (at - 1) % cuts, 1 - slot)

    finish(n - 1, cuts - 1, (n * cuts - 1) % 2)

    for p in range(n * cuts):
        for other, _ in others:
            pltpu.make_async_remote_copy(
                cross_out.at[p, 0], cross_in.at[p, other], cross_s.at[p, 0],
                cross_r.at[p, other], device_id=along_x, device_id_type=MESH,
            ).wait_recv()

    piece = 32

    @pl.loop(0, rows // piece)
    def _(i):
        at = pl.ds(pl.multiple_of(i * piece, piece), piece)
        blocks = []
        for p in range(n * cuts):
            total = fin[p, at, :]
            for other, _ in others:
                total = total + cross_in[p, other, at, :].astype(jnp.float32)
            blocks.append(total)
        square = sum(jnp.sum(b * b, axis=-1, keepdims=True) for b in blocks)
        scale = lax.rsqrt(square / (n * width) + EPS)
        for p in range(n * cuts):
            cols = pl.ds(p * sub, sub)
            out_ref[at, cols] = (blocks[p] * scale * post_ref[:, cols]).astype(out_ref.dtype)

    for i in range(8):
        token_send(i).wait_send()
    for s in range(n):
        for q in range(2 + cuts):
            @pl.when(has_right & (s <= k))
            def _():
                hop(0, s, q).wait_send()

            @pl.when(has_left & (s >= k))
            def _():
                hop(1, s, q).wait_send()
    for p in range(n * cuts):
        pair_copy(p).wait_send()
        for to, where in others:
            cross_copy(p, to, where).wait_send()


def chain_body(n, tokens, norm_gain, w_gate, w_up, w_down, post_gain):
    rows, model = tokens.shape
    depth, block = w_gate.shape
    width = w_down.shape[1]
    part = block // 2
    cuts = max(1, width // PIECE)
    sub = width // cuts
    vmem, dma = pltpu.VMEM, pltpu.SemaphoreType.DMA
    low, full = jnp.bfloat16, jnp.float32
    anywhere = pl.BlockSpec(memory_space=pl.ANY)
    inside = pl.BlockSpec(memory_space=vmem)
    return pl.pallas_call(
        functools.partial(kernel, n, rows, depth, part, width, cuts),
        out_shape=jax.ShapeDtypeStruct((rows, model), low),
        in_specs=[anywhere, inside, anywhere, anywhere, anywhere, inside],
        out_specs=inside,
        scratch_shapes=[
            vmem((8 * rows, model), low),
            vmem((8 * rows, model), low),
            vmem((8 * rows, 2 * part), full),
            vmem((n, depth, 2 * part), low),
            vmem((n, cuts, part, sub), low),
            vmem((8 * rows, part), low),
            vmem((2, 4, rows, sub), full),
            vmem((n * cuts, 4, rows, sub), low),
            vmem((n * cuts, 4, rows, sub), low),
            vmem((n * cuts, 4, rows, sub), low),
            vmem((n * cuts, 4, rows, sub), low),
            vmem((n * cuts, rows, sub), full),
            dma((3 + cuts,)),
            dma((8,)),
            dma((8,)),
            dma((2, n, 2 + cuts)),
            dma((n, 2 + cuts)),
            dma((n * cuts,)),
            dma((n * cuts,)),
            dma((n * cuts, 4)),
            dma((n * cuts, 4)),
        ],
        compiler_params=pltpu.CompilerParams(
            collective_id=0, has_side_effects=True, vmem_limit_bytes=56 * 2**20
        ),
    )(tokens, norm_gain.reshape(1, -1), w_gate, w_up, w_down, post_gain.reshape(1, -1))


def solution(mesh):
    n = mesh.shape["fs"]

    def body(tokens, norm_gain, w_gate, w_up, w_down, post_gain):
        args = (tokens, norm_gain, w_gate, w_up, w_down, post_gain)
        rows = tokens.shape[0]
        fits = (
            mesh.shape["rep"] == 2 and mesh.shape["tp"] == 4 and 2 <= n <= 4 and rows <= 128
            and rows % 64 == 0 and w_gate.shape[1] % 256 == 0 and w_down.shape[1] % PIECE == 0
        )
        return chain_body(n, *args) if fits else plain_body(*args)

    return jax.shard_map(
        body,
        mesh=mesh,
        in_specs=(
            P(("rep", "fs", "tp"), None),
            P(),
            P("fs", "tp"),
            P("fs", "tp"),
            P("tp", "fs"),
            P(),
        ),
        out_specs=P(("rep", "fs", "tp"), None),
        check_vma=False,
    )
```

```python
import functools

import jax
import jax.numpy as jnp
from jax import lax
from jax.experimental import pallas as pl
from jax.experimental.pallas import tpu as pltpu
from jax.sharding import PartitionSpec as P

EPS = 1e-06
MESH = pl.DeviceIdType.MESH
PIECE = 256


def rms_scale(values, gain):
    return values * lax.rsqrt(jnp.mean(values * values, axis=-1, keepdims=True) + EPS) * gain


def plain_body(tokens, norm_gain, w_gate, w_up, w_down, post_gain):
    own_normed = rms_scale(tokens.astype(jnp.float32), norm_gain).astype(jnp.bfloat16)
    normed = lax.all_gather(own_normed, "tp", axis=0, tiled=True)
    gate = jnp.dot(
        normed, lax.all_gather(w_gate, "fs", axis=0, tiled=True), preferred_element_type=jnp.float32
    )
    up = jnp.dot(
        normed, lax.all_gather(w_up, "fs", axis=0, tiled=True), preferred_element_type=jnp.float32
    )
    hidden = (jax.nn.silu(gate) * up).astype(jnp.bfloat16)
    terms = jnp.dot(
        hidden, lax.all_gather(w_down, "fs", axis=1, tiled=True), preferred_element_type=jnp.float32
    )
    summed = lax.psum_scatter(
        terms.astype(jnp.bfloat16), "tp", scatter_dimension=0, tiled=True
    ).astype(jnp.float32)
    return rms_scale(summed, post_gain).astype(jnp.bfloat16)


def kernel(
    n, rows, depth, part, width, cuts,
    tok_ref, gain_ref, wg_ref, wu_ref, wd_ref, post_ref, out_ref,
    raw, normed, acc, gu, dn, hidden, kept, pair_out, pair_in, cross_out, cross_in, fin,
    loc_sem, tok_s, tok_r, w_s, w_r, pair_s, pair_r, cross_s, cross_r,
):
    r, k, t = lax.axis_index("rep"), lax.axis_index("fs"), lax.axis_index("tp")
    x, c = t // 2, t % 2
    t_pair, t_x, r_y = x * 2 + (1 - c), (1 - x) * 2 + c, 1 - r
    partner, along_x, along_y, diag = {"tp": t_pair}, {"tp": t_x}, {"rep": r_y}, {"rep": r_y, "tp": t_x}
    has_left, has_right = k > 0, k < n - 1

    def weight(s, q):
        if isinstance(q, int) and q < 2:
            return gu.at[s, :, pl.ds(q * part, part)]
        return dn.at[s, q - 2]

    sub = width // cuts
    half = pl.multiple_of(r * part, part)
    loads = [
        pltpu.make_async_copy(wg_ref.at[:, pl.ds(half, part)], weight(k, 0), loc_sem.at[0]),
        pltpu.make_async_copy(wu_ref.at[:, pl.ds(half, part)], weight(k, 1), loc_sem.at[1]),
        pltpu.make_async_copy(tok_ref, raw.at[pl.ds((r * 4 + t) * rows, rows)], loc_sem.at[2]),
    ] + [
        pltpu.make_async_copy(
            wd_ref.at[pl.ds(half, part), pl.ds(j * sub, sub)], dn.at[k, j], loc_sem.at[3 + j]
        )
        for j in range(cuts)
    ]
    for load in loads:
        load.start()

    barrier = pltpu.get_barrier_semaphore()
    for where in (partner, along_x, along_y, diag):
        pl.semaphore_signal(barrier, inc=1, device_id=where, device_id_type=MESH)

    @pl.when(has_left)
    def _():
        pl.semaphore_signal(barrier, inc=1, device_id={"fs": k - 1}, device_id_type=MESH)

    @pl.when(has_right)
    def _():
        pl.semaphore_signal(barrier, inc=1, device_id={"fs": k + 1}, device_id_type=MESH)

    pl.semaphore_wait(barrier, 4 + jnp.where(has_left, 1, 0) + jnp.where(has_right, 1, 0))

    def remote(ref, send, recv, where):
        return pltpu.make_async_remote_copy(ref, ref, send, recv, device_id=where, device_id_type=MESH)

    def hop(way, s, q):
        return remote(weight(s, q), w_s.at[way, s, q], w_r.at[s, q], {"fs": k + 1 - 2 * way})

    def pass_on(way, s, q):
        @pl.when(has_left if way else has_right)
        def _():
            hop(way, s, q).start()

    def rows_of(r_at, t_at, first=0, count=rows):
        return raw.at[pl.ds((r_at * 4 + t_at) * rows + first, count)]

    upper = rows // 2
    token_sends = [
        (rows_of(r, t), partner),
        (rows_of(r, t), along_x),
        (rows_of(r, t), along_y),
        (rows_of(r, t_x, 0, upper), along_y),
        (rows_of(r_y, t, upper, upper), along_x),
        (rows_of(r, t_x), partner),
        (rows_of(r_y, t), partner),
        (rows_of(r_y, t_x), partner),
    ]
    t_px = (1 - x) * 2 + (1 - c)
    token_lands = [
        rows_of(r, t_pair),
        rows_of(r, t_x),
        rows_of(r_y, t),
        rows_of(r_y, t_x, 0, upper),
        rows_of(r_y, t_x, upper, upper),
        rows_of(r, t_px),
        rows_of(r_y, t_pair),
        rows_of(r_y, t_px),
    ]

    def token_send(i):
        ref, where = token_sends[i]
        return remote(ref, tok_s.at[i], tok_r.at[i], where)

    def token_wait(i):
        remote(token_lands[i], tok_s.at[i], tok_r.at[i], partner).wait_recv()

    loads[2].wait()
    for i in (1, 2, 0):
        token_send(i).start()
    for q in (0, 1):
        loads[q].wait()
        pass_on(0, k, q)
        pass_on(1, k, q)
    for load in loads[3:]:
        load.wait()

    def start_down(step):
        for way, distance in ((0, k), (1, n - 1 - k)):
            @pl.when(distance == step)
            def _():
                for j in range(cuts):
                    pass_on(way, k, 2 + j)

    start_down(0)

    def arrive(step, q):
        for way, s in ((0, k - step), (1, k + step)):
            @pl.when((s >= 0) if way == 0 else (s < n))
            def _():
                hop(way, s, q).wait_recv()
                pass_on(way, s, q)

    def forward_tokens():
        token_wait(1)
        token_send(3).start()
        token_send(5).start()
        token_wait(2)
        token_send(4).start()
        token_send(6).start()

    def finish_tokens():
        token_wait(3)
        token_wait(4)
        token_send(7).start()
        for i in (0, 5, 6, 7):
            token_wait(i)

        tile = 32

        @pl.loop(0, 8 * rows // tile)
        def _(i):
            at = pl.ds(pl.multiple_of(i * tile, tile), tile)
            normed[at, :] = rms_scale(raw[at, :].astype(jnp.float32), gain_ref[...]).astype(jnp.bfloat16)

    tile = 2 * rows

    def add_block(s, first):
        cols = pl.ds(pl.multiple_of(s * depth, depth), depth)

        @pl.loop(0, 4)
        def _(i):
            at = pl.ds(pl.multiple_of(i * tile, tile), tile)
            term = jnp.dot(normed[at, cols], gu[s], preferred_element_type=jnp.float32)
            acc[at, :] = term if first else acc[at, :] + term

    for step in range(1, n):
        arrive(step, 0)
        if step == 1:
            forward_tokens()
        arrive(step, 1)
        start_down(step)
        if step == 1:
            finish_tokens()
            add_block(k, True)
        for s in (k - step, k + step):
            @pl.when((s >= 0) & (s < n))
            def _():
                add_block(s, False)

    @pl.loop(0, 16)
    def _(i):
        at = pl.ds(pl.multiple_of(i * (rows // 2), rows // 2), rows // 2)
        gate, up = acc[at, :part], acc[at, part:]
        hidden[at, :] = (gate / (1.0 + jnp.exp(-gate)) * up).astype(jnp.bfloat16)

    mine = r * 2 + x
    others = ((r * 2 + (1 - x), along_x), (r_y * 2 + x, along_y), (r_y * 2 + (1 - x), diag))

    def pair_copy(p):
        return pltpu.make_async_remote_copy(
            pair_out.at[p], pair_in.at[p], pair_s.at[p], pair_r.at[p], device_id=partner, device_id_type=MESH
        )

    def cross_copy(p, to, where):
        return pltpu.make_async_remote_copy(
            cross_out.at[p, to], cross_in.at[p, mine], cross_s.at[p, to], cross_r.at[p, mine],
            device_id=where, device_id_type=MESH,
        )

    both_ways = jnp.minimum(k, n - 1 - k)
    far = jnp.where(k < n - 1 - k, 1, -1)

    def source(i):
        near = jnp.where(i % 2 == 1, k - (i + 1) // 2, k + i // 2)
        return jnp.where(i <= 2 * both_ways, near, k + far * (i - both_ways))

    def product(m, core, s, j):
        at = pl.ds(pl.multiple_of((m * 2 + core) * rows, rows), rows)
        return jnp.dot(hidden[at, :], dn[s, j], preferred_element_type=jnp.float32)

    def finish(i, j, slot):
        p = source(i) * cuts + j
        pair_copy(p).wait_recv()
        for to, where in (others[2], others[0], others[1]):
            cross_out[p, to] = (kept[slot, to] + pair_in[p, to].astype(jnp.float32)).astype(jnp.bfloat16)
        for to, where in (others[2], others[0], others[1]):
            cross_copy(p, to, where).start()
        fin[p] = kept[slot, mine] + pair_in[p, mine].astype(jnp.float32)

    @pl.loop(0, n * cuts)
    def _(at):
        i, j, slot = at // cuts, at % cuts, at % 2
        s = source(i)
        p = s * cuts + j

        @pl.when(at > 0)
        def _():
            finish((at - 1) // cuts, (at - 1) % cuts, 1 - slot)

        @pl.when(i > 0)
        def _():
            remote(dn.at[s, j], w_s.at[0, s, 2 + j], w_r.at[s, 2 + j], partner).wait_recv()

        @pl.when((i > 0) & (s < k))
        def _():
            pass_on(0, s, 2 + j)

        @pl.when((i > 0) & (s > k))
        def _():
            pass_on(1, s, 2 + j)

        @pl.loop(0, 4)
        def _(m):
            pair_out[p, m] = product(m, 1 - c, s, j).astype(jnp.bfloat16)

        pair_copy(p).start()

        @pl.loop(0, 4)
        def _(m):
            kept[slot, m] = product(m, c, s, j)

    finish(n - 1, cuts - 1, (n * cuts - 1) % 2)

    for p in range(n * cuts):
        for other, _ in others:
            pltpu.make_async_remote_copy(
                cross_out.at[p, 0], cross_in.at[p, other], cross_s.at[p, 0],
                cross_r.at[p, other], device_id=along_x, device_id_type=MESH,
            ).wait_recv()

    piece = 32

    @pl.loop(0, rows // piece)
    def _(i):
        at = pl.ds(pl.multiple_of(i * piece, piece), piece)
        blocks = []
        for p in range(n * cuts):
            total = fin[p, at, :]
            for other, _ in others:
                total = total + cross_in[p, other, at, :].astype(jnp.float32)
            blocks.append(total)
        square = sum(jnp.sum(b * b, axis=-1, keepdims=True) for b in blocks)
        scale = lax.rsqrt(square / (n * width) + EPS)
        for p in range(n * cuts):
            cols = pl.ds(p * sub, sub)
            out_ref[at, cols] = (blocks[p] * scale * post_ref[:, cols]).astype(out_ref.dtype)

    for i in range(8):
        token_send(i).wait_send()
    for s in range(n):
        for q in range(2 + cuts):
            @pl.when(has_right & (s <= k))
            def _():
                hop(0, s, q).wait_send()

            @pl.when(has_left & (s >= k))
            def _():
                hop(1, s, q).wait_send()
    for p in range(n * cuts):
        pair_copy(p).wait_send()
        for to, where in others:
            cross_copy(p, to, where).wait_send()


def chain_body(n, tokens, norm_gain, w_gate, w_up, w_down, post_gain):
    rows, model = tokens.shape
    depth, block = w_gate.shape
    width = w_down.shape[1]
    part = block // 2
    cuts = max(1, width // PIECE)
    sub = width // cuts
    vmem, dma = pltpu.VMEM, pltpu.SemaphoreType.DMA
    low, full = jnp.bfloat16, jnp.float32
    anywhere = pl.BlockSpec(memory_space=pl.ANY)
    inside = pl.BlockSpec(memory_space=vmem)
    return pl.pallas_call(
        functools.partial(kernel, n, rows, depth, part, width, cuts),
        out_shape=jax.ShapeDtypeStruct((rows, model), low),
        in_specs=[anywhere, inside, anywhere, anywhere, anywhere, inside],
        out_specs=inside,
        scratch_shapes=[
            vmem((8 * rows, model), low),
            vmem((8 * rows, model), low),
            vmem((8 * rows, 2 * part), full),
            vmem((n, depth, 2 * part), low),
            vmem((n, cuts, part, sub), low),
            vmem((8 * rows, part), low),
            vmem((2, 4, rows, sub), full),
            vmem((n * cuts, 4, rows, sub), low),
            vmem((n * cuts, 4, rows, sub), low),
            vmem((n * cuts, 4, rows, sub), low),
            vmem((n * cuts, 4, rows, sub), low),
            vmem((n * cuts, rows, sub), full),
            dma((3 + cuts,)),
            dma((8,)),
            dma((8,)),
            dma((2, n, 2 + cuts)),
            dma((n, 2 + cuts)),
            dma((n * cuts,)),
            dma((n * cuts,)),
            dma((n * cuts, 4)),
            dma((n * cuts, 4)),
        ],
        compiler_params=pltpu.CompilerParams(
            collective_id=0, has_side_effects=True, vmem_limit_bytes=56 * 2**20
        ),
    )(tokens, norm_gain.reshape(1, -1), w_gate, w_up, w_down, post_gain.reshape(1, -1))


def solution(mesh):
    n = mesh.shape["fs"]

    def body(tokens, norm_gain, w_gate, w_up, w_down, post_gain):
        args = (tokens, norm_gain, w_gate, w_up, w_down, post_gain)
        rows = tokens.shape[0]
        fits = (
            mesh.shape["rep"] == 2 and mesh.shape["tp"] == 4 and 2 <= n <= 4 and rows <= 128
            and rows % 64 == 0 and w_gate.shape[1] % 256 == 0 and w_down.shape[1] % PIECE == 0
        )
        return chain_body(n, *args) if fits else plain_body(*args)

    return jax.shard_map(
        body,
        mesh=mesh,
        in_specs=(
            P(("rep", "fs", "tp"), None),
            P(),
            P("fs", "tp"),
            P("fs", "tp"),
            P("tp", "fs"),
            P(),
        ),
        out_specs=P(("rep", "fs", "tp"), None),
        check_vma=False,
    )
```
